32 devices in a mesh: sp: 32 (over z, y, x, core), tp: 1.
Axes of the slice: x: 2, y: 2, z: 4, core: 2. Of those that a mesh axis runs over, the one named last changes fastest.
Arguments:
- stream: bfloat16 [8192, 2048], P(('sp', 'tp')), may hold values from -6 to 6
- query_one: bfloat16 [8192, 512], P('sp', 'tp'), may hold values from -280 to 280
- key_one: bfloat16 [8192, 512], P('sp', 'tp'), may hold values from -6 to 6
- query_two: bfloat16 [8192, 512], P('sp', 'tp'), may hold values from -280 to 280
- key_two: bfloat16 [8192, 512], P('sp', 'tp'), may hold values from -6 to 6
- values: bfloat16 [8192, 1024], P('sp', 'tp'), may hold values from -6 to 6
- lambdas: float32 [8], P('tp'), may hold values from 0.3 to 0.8
- head_gain: float32 [128], replicated, may hold values from 0.1 to 1.9
- out_weight: bfloat16 [1024, 2048], replicated, may hold values from -0.1875 to 0.1875
- norm_gain: float32 [2048], replicated, may hold values from 0.1 to 1.9
- gate_weight: bfloat16 [2048, 2816], P('sp', 'tp'), may hold values from -0.125 to 0.125
- up_weight: bfloat16 [2048, 2816], P('sp', 'tp'), may hold values from -0.125 to 0.125
- down_weight: bfloat16 [2816, 2048], P('tp', 'sp'), may hold values from -0.3125 to 0.3125
Outputs:
- result: bfloat16 [8192, 2048], P(('sp', 'tp'))
The draws below stay inside these ranges and needn't reach their ends.
All inputs are finite; a program needn't handle non-finite values.
Results may differ from the reference program's by a relative error of at most 0.014.
Values may be sent and summed in bfloat16 or wider, within the bound.
No kernel may reach another device: no remote copies, remote signals or barrier semaphores. Data moves between devices by JAX's collectives and lax.ppermute only.
A program may use at most 192 MiB of HBM per device.

```python
import jax
import jax.numpy as jnp
from jax import lax

D = 2048
HEADS = 8
HEAD_DIM = 64
VDIM = 128
FF = 2816
SEQ = 8192
N_TP = 1


def drawn_pair(key, tag):
    folded = jax.random.fold_in(key, tag)
    query_seed, key_seed = jax.random.split(folded)
    row_width = HEADS * HEAD_DIM
    queries = jnp.clip(jax.random.normal(query_seed, (SEQ, row_width), jnp.float32), -6.0, 6.0) * 1.75
    keys = jnp.clip(jax.random.normal(key_seed, (SEQ, row_width), jnp.float32), -6.0, 6.0)
    return (queries, keys)


def draw_query_one(key, part):
    return drawn_pair(key, 11)[0].astype(jnp.bfloat16)


def draw_key_one(key, part):
    return drawn_pair(key, 11)[1].astype(jnp.bfloat16)


def draw_query_two(key, part):
    return drawn_pair(key, 23)[0].astype(jnp.bfloat16)


def draw_key_two(key, part):
    return drawn_pair(key, 23)[1].astype(jnp.bfloat16)


def block_scale(key, extent, pieces, least, largest):
    factor_of, own = 1.0, jax.random.fold_in(key, 6)
    for axis_at, blocks in pieces:
        steps = jnp.exp(jax.random.uniform(jax.random.fold_in(own, axis_at), (blocks,), jnp.float32, least / len(pieces), largest / len(pieces)))
        factor_of = factor_of * jnp.repeat(steps, extent[axis_at] // blocks).reshape([-1 if axis == axis_at else 1 for axis in range(len(extent))])
    return factor_of


def noise(key, extent, width, bound, cuts=(), kind=jnp.bfloat16):
    values = width * jax.random.normal(key, extent, jnp.float32)
    if cuts:
        values = values * block_scale(key, extent, cuts, -0.22, 0.18)
    return jnp.clip(values, -bound, bound).astype(kind)


def setup_inputs(seed: int = 0) -> dict:
    key_of = jax.random.split(jax.random.key(seed), 14)
    return {
        "stream": noise(key_of[0], (SEQ, D), 1.0, 6.0, ((0, 32),)),
        "query_one": draw_query_one(jax.random.fold_in(key_of[13], 71), 0),
        "key_one": draw_key_one(jax.random.fold_in(key_of[13], 71), 0),
        "query_two": draw_query_two(jax.random.fold_in(key_of[13], 71), 0),
        "key_two": draw_key_two(jax.random.fold_in(key_of[13], 71), 0),
        "values": noise(key_of[5], (SEQ, HEADS * VDIM), 1.0, 6.0, ((0, 32),)),
        "lambdas": jnp.clip(jax.random.uniform(key_of[6], (HEADS,), jnp.float32, 0.3, 0.8), 0.3, 0.8),
        "head_gain": jnp.clip(1.0 + 0.18 * jax.random.normal(key_of[7], (VDIM,), jnp.float32), 0.1, 1.9),
        "out_weight": noise(key_of[8], (HEADS * VDIM, D), (HEADS * VDIM) ** -0.5, 0.1875),
        "norm_gain": jnp.clip(1.0 + 0.18 * jax.random.normal(key_of[9], (D,), jnp.float32), 0.1, 1.9),
        "gate_weight": noise(key_of[10], (D, FF), D ** -0.5, 0.125, ((0, 32),)),
        "up_weight": noise(key_of[11], (D, FF), D ** -0.5, 0.125, ((0, 32),)),
        "down_weight": noise(key_of[12], (FF, D), (FF // 9) ** -0.5, 0.3125, ((1, 32),)),
    }


ALPHA = 1.4142135623730951
EPSILON = 1e-05

def one_map(queries, keys, value_rows):
    factor = HEAD_DIM ** (-0.5)
    scores = jnp.einsum('qhd,khd->hqk', queries.astype(jnp.float32), keys.astype(jnp.float32)) * factor
    row_peak = lax.optimization_barrier(jnp.max(scores, axis=-1, keepdims=True))
    weights = jnp.exp(scores - row_peak)
    totals = lax.optimization_barrier(jnp.sum(weights, axis=-1))
    rounded = lax.optimization_barrier(weights.astype(jnp.bfloat16))
    summed = jnp.einsum('hqk,khe->qhe', rounded.astype(jnp.float32), value_rows.astype(jnp.float32))
    return summed / jnp.transpose(totals)[:, :, None]

def layer_normed(heads_rows, residual_rows, out_weight, norm_gain):
    branch = jnp.dot(heads_rows, out_weight, preferred_element_type=jnp.float32)
    mixed_in = ALPHA * residual_rows.astype(jnp.float32) + branch
    row_mean = lax.optimization_barrier(jnp.mean(mixed_in, axis=-1, keepdims=True))
    centered = mixed_in - row_mean
    row_var = lax.optimization_barrier(jnp.mean(centered * centered, axis=-1, keepdims=True))
    return (centered * lax.rsqrt(row_var + EPSILON) * norm_gain).astype(jnp.bfloat16)

def reference(stream, query_one, key_one, query_two, key_two, values, lambdas, head_gain, out_weight, norm_gain, gate_weight, up_weight, down_weight):
    keys_first = key_one.reshape(SEQ, HEADS, HEAD_DIM)
    keys_second = key_two.reshape(SEQ, HEADS, HEAD_DIM)
    value_rows = values.reshape(SEQ, HEADS, VDIM)
    block_rows = 256
    block_count = SEQ // block_rows

    def attend(position):
        begin_row = position * block_rows
        first_rows = lax.dynamic_slice_in_dim(query_one, begin_row, block_rows, 0).reshape(block_rows, HEADS, HEAD_DIM)
        second_rows = lax.dynamic_slice_in_dim(query_two, begin_row, block_rows, 0).reshape(block_rows, HEADS, HEAD_DIM)
        first_map = one_map(first_rows, keys_first, value_rows)
        second = one_map(second_rows, keys_second, value_rows)
        differ = first_map - lambdas[None, :, None] * second
        inverse_rms = lax.rsqrt(lax.optimization_barrier(jnp.mean(differ * differ, axis=-1, keepdims=True)) + EPSILON)
        return (differ * inverse_rms * head_gain * 0.8).astype(jnp.bfloat16).reshape(block_rows, HEADS * VDIM)
    attended = lax.map(attend, jnp.arange(block_count, dtype=jnp.int32)).reshape(SEQ, HEADS * VDIM)
    normed = layer_normed(attended, stream, out_weight, norm_gain)
    gate_out = jnp.dot(normed, gate_weight, preferred_element_type=jnp.float32)
    upward = jnp.dot(normed, up_weight, preferred_element_type=jnp.float32)
    hidden = (jax.nn.silu(gate_out) * upward).astype(jnp.bfloat16)
    group_width = FF // N_TP
    mixer_out = jnp.zeros((SEQ, D), jnp.float32)
    for group_index in range(N_TP):
        low_unit = group_index * group_width
        partial_value = jnp.dot(hidden[:, low_unit:low_unit + group_width], down_weight[low_unit:low_unit + group_width, :], preferred_element_type=jnp.float32)
        partial_value = lax.optimization_barrier(partial_value.astype(jnp.bfloat16))
        mixer_out = mixer_out + partial_value.astype(jnp.float32)
    return (ALPHA * normed.astype(jnp.float32) + 0.5 * mixer_out).astype(jnp.bfloat16)
```

```python
import functools
import math

import jax
import jax.numpy as jnp
from jax import lax
from jax.experimental import pallas as pl
from jax.experimental.pallas import tpu as pltpu
from jax.sharding import PartitionSpec as P

ALPHA = 1.4142135623730951
EPSILON = 1e-05
LOG2E = 1.4426950408889634
VMEM_LIMIT = 60 * 1024 * 1024


def pack_kernel(q1, q2, k1, k2, v, out, *, heads, hd, vd):
    for h in range(heads):
        cols = slice(h * hd, (h + 1) * hd)
        out[0, h] = jnp.concatenate([q1[:, cols], q2[:, cols]], axis=1)
        out[1, h] = jnp.concatenate([k1[:, cols], k2[:, cols]], axis=1)
        out[2, h] = v[:, h * vd : (h + 1) * vd]


def pack(q1, q2, k1, k2, v, heads):
    rows = q1.shape[0]
    hd, vd = q1.shape[1] // heads, v.shape[1] // heads
    return pl.pallas_call(
        functools.partial(pack_kernel, heads=heads, hd=hd, vd=vd),
        out_shape=jax.ShapeDtypeStruct((3, heads, rows, vd), jnp.bfloat16),
        compiler_params=pltpu.CompilerParams(vmem_limit_bytes=VMEM_LIMIT),
    )(q1, q2, k1, k2, v)


def attend_kernel(*refs, kb, hd, first, last):
    refs = list(refs)
    q_ref, k_ref, v_ref = refs[:3]
    refs = refs[3:]
    if not first:
        m_in, l_in, o_in = refs[:3]
        refs = refs[3:]
    if last:
        lam_ref, gain_ref, out_ref, vt_ref = refs
    else:
        m_out, l_out, o_out, vt_ref = refs
    qb, kc, vd = q_ref.shape[0], k_ref.shape[0], v_ref.shape[1]
    c = LOG2E * hd**-0.5

    @pl.when(pl.program_id(0) == 0)
    def _():
        vt_ref[...] = v_ref[...].T

    qt = q_ref[...].T
    row = lax.broadcasted_iota(jnp.int32, qt.shape, 0)
    zero = jnp.zeros_like(qt)
    queries = (jnp.where(row < hd, qt, zero), jnp.where(row >= hd, qt, zero))
    state = []
    for a in (0, 1):
        cols = slice(a * qb, (a + 1) * qb)
        if first:
            state.append(
                (
                    jnp.full((1, qb), -1e30, jnp.float32),
                    jnp.zeros((1, qb), jnp.float32),
                    jnp.zeros((vd, qb), jnp.float32),
                )
            )
        else:
            state.append((m_in[:, cols], l_in[:, cols], o_in[:, cols]))

    def scores(step):
        j, a = step
        return jnp.dot(
            k_ref[j * kb : (j + 1) * kb, :], queries[a], preferred_element_type=jnp.float32
        )

    steps = [(j, a) for j in range(kc // kb) for a in (0, 1)]
    s = scores(steps[0])
    for t, (j, a) in enumerate(steps):
        s_next = scores(steps[t + 1]) if t + 1 < len(steps) else None
        m, l, o = state[a]
        m_new = jnp.maximum(m, jnp.max(s, axis=0, keepdims=True))
        p = jnp.exp2((s - m_new) * c)
        scale = jnp.exp2((m - m_new) * c)
        l = l * scale + jnp.sum(p, axis=0, keepdims=True)
        o = o * scale + jnp.dot(
            vt_ref[:, j * kb : (j + 1) * kb],
            p.astype(jnp.bfloat16),
            preferred_element_type=jnp.float32,
        )
        state[a] = (m_new, l, o)
        s = s_next
    if last:
        first_map = state[0][2] / state[0][1]
        second_map = state[1][2] / state[1][1]
        differ = first_map - lam_ref[0, 0] * second_map
        inverse = lax.rsqrt(jnp.mean(differ * differ, axis=0, keepdims=True) + EPSILON)
        attended = differ * inverse * gain_ref[...] * 0.8
        out_ref[...] = attended.T.astype(jnp.bfloat16)
    else:
        for a in (0, 1):
            cols = slice(a * qb, (a + 1) * qb)
            m_out[:, cols], l_out[:, cols], o_out[:, cols] = state[a]


def attend(q, k, v, state, final, hd):
    nq, kc, vd = q.shape[0], k.shape[0], v.shape[1]
    qb = math.gcd(nq, 512)
    kb = math.gcd(kc, 1024)
    wide = lambda r: pl.BlockSpec((r, 2 * qb), lambda i: (0, i))
    whole = lambda a: pl.BlockSpec(a.shape, lambda i: (0, 0))
    args = [q, k, v]
    in_specs = [pl.BlockSpec((qb, q.shape[1]), lambda i: (i, 0)), whole(k), whole(v)]
    aliases = {}
    if state is not None:
        args += list(state)
        in_specs += [wide(1), wide(1), wide(vd)]
    if final is not None:
        lam, gain = final
        args += [lam, gain]
        in_specs += [pl.BlockSpec(memory_space=pltpu.SMEM), whole(gain)]
        out_shape = jax.ShapeDtypeStruct((nq, vd), jnp.bfloat16)
        out_specs = pl.BlockSpec((qb, vd), lambda i: (i, 0))
    else:
        out_shape = [jax.ShapeDtypeStruct((r, 2 * nq), jnp.float32) for r in (1, 1, vd)]
        out_specs = [wide(1), wide(1), wide(vd)]
        if state is not None:
            aliases = {3: 0, 4: 1, 5: 2}
    scores = 2 * nq * kc
    return pl.pallas_call(
        functools.partial(
            attend_kernel, kb=kb, hd=hd, first=state is None, last=final is not None
        ),
        grid=(nq // qb,),
        in_specs=in_specs,
        out_specs=out_specs,
        out_shape=out_shape,
        input_output_aliases=aliases,
        scratch_shapes=[pltpu.VMEM((vd, kc), jnp.bfloat16)],
        compiler_params=pltpu.CompilerParams(
            dimension_semantics=("arbitrary",), vmem_limit_bytes=VMEM_LIMIT
        ),
        cost_estimate=pl.CostEstimate(
            flops=2 * scores * (hd + vd), transcendentals=scores, bytes_accessed=4 * nq * vd * 4
        ),
    )(*args)


def layer_normed(heads_rows, residual_rows, out_weight, norm_gain):
    branch = jnp.dot(heads_rows, out_weight, preferred_element_type=jnp.float32)
    mixed_in = ALPHA * residual_rows.astype(jnp.float32) + branch
    row_mean = jnp.mean(mixed_in, axis=-1, keepdims=True)
    centered = mixed_in - row_mean
    row_var = jnp.mean(centered * centered, axis=-1, keepdims=True)
    return (centered * lax.rsqrt(row_var + EPSILON) * norm_gain).astype(jnp.bfloat16)


def attention(query_one, key_one, query_two, key_two, values, lambdas, head_gain):
    heads = lambdas.shape[0]
    tokens = query_one.shape[0]
    hd, vd = query_one.shape[1] // heads, values.shape[1] // heads
    group = lax.axis_size("sp")
    share = group // heads
    part = tokens // share
    packed = pack(query_one, query_two, key_one, key_two, values, heads)
    packed = packed.reshape(3, group, part, vd)
    mine = lax.all_to_all(packed, "sp", split_axis=1, concat_axis=1, tiled=True)
    mine = mine.reshape(3, group * part, vd)
    chunks = {0: mine[1:]}
    for mask in range(1, share):
        low = mask & -mask
        ring = [(i, i ^ low) for i in range(group)]
        chunks[mask] = lax.ppermute(chunks[mask - low], "sp", ring)
    head = lax.axis_index("sp") // share
    lam = lax.dynamic_slice_in_dim(lambdas, head, 1).reshape(1, 1)
    final = (lam, head_gain.reshape(vd, 1))
    order = [0, 1] + list(range(2, share)) if share > 1 else [0]
    state = None
    for n, mask in enumerate(order):
        kv = chunks[mask]
        state = attend(
            mine[0], kv[0], kv[1], state, final if n + 1 == len(order) else None, hd
        )
    back = lax.all_to_all(
        state.reshape(group, part, vd), "sp", split_axis=0, concat_axis=0, tiled=True
    )
    return (
        back.reshape(heads, share, part, vd)
        .transpose(1, 2, 0, 3)
        .reshape(tokens, heads * vd)
    )


def on_device(
    stream,
    query_one,
    key_one,
    query_two,
    key_two,
    values,
    lambdas,
    head_gain,
    out_weight,
    norm_gain,
    gate_weight,
    up_weight,
    down_weight,
):
    gate_full = lax.all_gather(gate_weight, "sp", axis=0, tiled=True)
    up_full = lax.all_gather(up_weight, "sp", axis=0, tiled=True)
    down_full = lax.all_gather(down_weight.T, "sp", axis=0, tiled=True)
    attended = attention(
        query_one, key_one, query_two, key_two, values, lambdas, head_gain
    )
    by_rows = lax.all_to_all(attended, "tp", split_axis=0, concat_axis=1, tiled=True)
    own_normed = layer_normed(by_rows, stream, out_weight, norm_gain)
    normed_all = lax.all_gather(own_normed, "tp", axis=0, tiled=True)
    gate_out = jnp.dot(normed_all, gate_full, preferred_element_type=jnp.float32)
    upward = jnp.dot(normed_all, up_full, preferred_element_type=jnp.float32)
    hidden = (jax.nn.silu(gate_out) * upward).astype(jnp.bfloat16)
    partial_terms = lax.dot_general(
        hidden, down_full, (((1,), (1,)), ((), ())), preferred_element_type=jnp.float32
    )
    mixer_out = lax.psum_scatter(
        partial_terms.astype(jnp.bfloat16), "tp", scatter_dimension=0, tiled=True
    ).astype(jnp.float32)
    return (ALPHA * own_normed.astype(jnp.float32) + 0.5 * mixer_out).astype(jnp.bfloat16)


def solution(mesh):
    return jax.shard_map(
        on_device,
        mesh=mesh,
        in_specs=(
            P(("sp", "tp"), None),
            P("sp", "tp"),
            P("sp", "tp"),
            P("sp", "tp"),
            P("sp", "tp"),
            P("sp", "tp"),
            P("tp"),
            P(),
            P(),
            P(),
            P("sp", "tp"),
            P("sp", "tp"),
            P("tp", "sp"),
        ),
        out_specs=P(("sp", "tp"), None),
        check_vma=False,
    )
```

```python
import functools
import math

import jax
import jax.numpy as jnp
from jax import lax
from jax.experimental import pallas as pl
from jax.experimental.pallas import tpu as pltpu
from jax.sharding import PartitionSpec as P

ALPHA = 1.4142135623730951
EPSILON = 1e-05
LOG2E = 1.4426950408889634
VMEM_LIMIT = 60 * 1024 * 1024


def pack_kernel(q1, q2, k1, k2, v, out, *, heads, hd, vd):
    for h in range(heads):
        cols = slice(h * hd, (h + 1) * hd)
        out[h, 0] = jnp.concatenate([q1[:, cols], q2[:, cols]], axis=1)
        out[h, 1] = jnp.concatenate([k1[:, cols], k2[:, cols]], axis=1)
        out[h, 2] = v[:, h * vd : (h + 1) * vd]


def pack(q1, q2, k1, k2, v, heads):
    rows = q1.shape[0]
    hd, vd = q1.shape[1] // heads, v.shape[1] // heads
    return pl.pallas_call(
        functools.partial(pack_kernel, heads=heads, hd=hd, vd=vd),
        out_shape=jax.ShapeDtypeStruct((heads, 3, rows, vd), jnp.bfloat16),
        compiler_params=pltpu.CompilerParams(vmem_limit_bytes=VMEM_LIMIT),
    )(q1, q2, k1, k2, v)


def pack_weights_kernel(place, gate, up, down, *outs_and_buf):
    outs, buf = outs_and_buf[:-1], outs_and_buf[-1]
    width = gate.shape[1] // len(outs)
    for p in range(len(outs)):
        cols = slice(p * width, (p + 1) * width)
        slot = jnp.bitwise_xor(place[0], p)
        buf[slot, 0] = gate[:, cols]
        buf[slot, 1] = up[:, cols]
        buf[slot, 2] = down[cols, :].T
    for p, out in enumerate(outs):
        out[...] = buf[p]


def pack_weights(place, gate, up, down, parts):
    rows, ff = gate.shape
    piece = (3, rows, ff // parts)
    return pl.pallas_call(
        pack_weights_kernel,
        in_specs=[pl.BlockSpec(memory_space=pltpu.SMEM)] + [pl.BlockSpec()] * 3,
        out_shape=[jax.ShapeDtypeStruct(piece, jnp.bfloat16)] * parts,
        scratch_shapes=[pltpu.VMEM((parts,) + piece, jnp.bfloat16)],
        compiler_params=pltpu.CompilerParams(vmem_limit_bytes=VMEM_LIMIT),
    )(place, gate, up, down)


def assemble_kernel(place, *refs):
    parts, out = refs[:-1], refs[-1]
    rows = parts[0].shape[1]
    for p, part in enumerate(parts):
        at = pl.multiple_of(jnp.bitwise_xor(place[0], p) * rows, rows)
        out[:, pl.ds(at, rows), :] = part[...]


def assemble(place, parts):
    kinds, rows, width = parts[0].shape
    return pl.pallas_call(
        assemble_kernel,
        in_specs=[pl.BlockSpec(memory_space=pltpu.SMEM)] + [pl.BlockSpec()] * len(parts),
        out_shape=jax.ShapeDtypeStruct((kinds, len(parts) * rows, width), jnp.bfloat16),
        compiler_params=pltpu.CompilerParams(vmem_limit_bytes=VMEM_LIMIT),
    )(place, *parts)


def mixer_kernel(base, *refs, masks, far, rows):
    weights = refs[: len(masks)]
    xa, xb, out_a, out_b, buf, sems = refs[len(masks) :]
    kinds = (slice(0, 2), slice(2, 3))

    def copies(part):
        for m, mask in enumerate(masks):
            for n, f in enumerate((0, far)):
                at = (jnp.bitwise_xor(base[0], mask) + f) * rows
                at = pl.multiple_of(at, 2 * rows)
                yield pltpu.make_async_copy(
                    weights[m].at[kinds[part], pl.ds(n * 2 * rows, 2 * rows)],
                    buf.at[kinds[part], pl.ds(at, 2 * rows)],
                    sems.at[part, 2 * m + n],
                )

    for part in (0, 1):
        for copy in copies(part):
            copy.start()
    for copy in copies(0):
        copy.wait()
    hidden = []
    for x in (xa, xb):
        gate = jnp.dot(x[...], buf[0], preferred_element_type=jnp.float32)
        up = jnp.dot(x[...], buf[1], preferred_element_type=jnp.float32)
        hidden.append((gate / (1.0 + jnp.exp(-gate)) * up).astype(jnp.bfloat16))
    for copy in copies(1):
        copy.wait()
    for h, out in zip(hidden, (out_a, out_b)):
        out[...] = lax.dot_general(
            h, buf[2], (((1,), (1,)), ((), ())), preferred_element_type=jnp.float32
        ).astype(jnp.bfloat16)


def mixer(base, xa, xb, weights, masks, far):
    kinds, block, width = weights[0].shape
    n, d = xa.shape
    return pl.pallas_call(
        functools.partial(mixer_kernel, masks=masks, far=far, rows=block // 4),
        in_specs=[pl.BlockSpec(memory_space=pltpu.SMEM)]
        + [pl.BlockSpec(memory_space=pl.ANY)] * len(masks)
        + [pl.BlockSpec()] * 2,
        out_shape=[jax.ShapeDtypeStruct((n, d), jnp.bfloat16)] * 2,
        scratch_shapes=[
            pltpu.VMEM((kinds, d, width), jnp.bfloat16),
            pltpu.SemaphoreType.DMA((2, 2 * len(masks))),
        ],
        compiler_params=pltpu.CompilerParams(vmem_limit_bytes=VMEM_LIMIT),
        cost_estimate=pl.CostEstimate(
            flops=12 * n * d * width,
            transcendentals=2 * n * width,
            bytes_accessed=2 * kinds * d * width,
        ),
    )(base, *weights, xa, xb)


def attend_kernel(*refs, kb, hd, first, last):
    refs = list(refs)
    q_ref, k_ref, v_ref = refs[:3]
    refs = refs[3:]
    if not first:
        m_in, l_in, o_in = refs[:3]
        refs = refs[3:]
    if last:
        lam_ref, gain_ref, out_ref, vt_ref = refs
    else:
        m_out, l_out, o_out, vt_ref = refs
    vd = q_ref.shape[-1]
    qb = q_ref.shape[0] * q_ref.shape[2]
    kc = k_ref.shape[0] * k_ref.shape[2]
    c = LOG2E * hd**-0.5
    keys = k_ref.reshape(kc, vd)

    @pl.when(pl.program_id(0) == 0)
    def _():
        vt_ref[...] = v_ref[...].reshape(kc, vd).T

    qt = q_ref[...].reshape(qb, vd).T
    row = lax.broadcasted_iota(jnp.int32, qt.shape, 0)
    zero = jnp.zeros_like(qt)
    queries = (jnp.where(row < hd, qt, zero), jnp.where(row >= hd, qt, zero))
    state = []
    for a in (0, 1):
        cols = slice(a * qb, (a + 1) * qb)
        if first:
            state.append(
                (
                    jnp.full((1, qb), -1e30, jnp.float32),
                    jnp.zeros((1, qb), jnp.float32),
                    jnp.zeros((vd, qb), jnp.float32),
                )
            )
        else:
            state.append((m_in[:, cols], l_in[:, cols], o_in[:, cols]))

    def scores(step):
        j, a = step
        return jnp.dot(
            keys[j * kb : (j + 1) * kb, :], queries[a], preferred_element_type=jnp.float32
        )

    steps = [(j, a) for j in range(kc // kb) for a in (0, 1)]
    s = scores(steps[0])
    for t, (j, a) in enumerate(steps):
        s_next = scores(steps[t + 1]) if t + 1 < len(steps) else None
        m, l, o = state[a]
        m_new = jnp.maximum(m, jnp.max(s, axis=0, keepdims=True))
        p = jnp.exp2((s - m_new) * c)
        scale = jnp.exp2((m - m_new) * c)
        l = l * scale + jnp.sum(p, axis=0, keepdims=True)
        o = o * scale + jnp.dot(
            vt_ref[:, j * kb : (j + 1) * kb],
            p.astype(jnp.bfloat16),
            preferred_element_type=jnp.float32,
        )
        state[a] = (m_new, l, o)
        s = s_next
    if last:
        first_map = state[0][2] / state[0][1]
        second_map = state[1][2] / state[1][1]
        differ = first_map - lam_ref[0, 0] * second_map
        inverse = lax.rsqrt(jnp.mean(differ * differ, axis=0, keepdims=True) + EPSILON)
        attended = differ * inverse * gain_ref[...] * 0.8
        out_ref[...] = attended.T.astype(jnp.bfloat16)
    else:
        for a in (0, 1):
            cols = slice(a * qb, (a + 1) * qb)
            m_out[:, cols], l_out[:, cols], o_out[:, cols] = state[a]


def attend(q, kv, state, final, hd):
    blocks, _, rows, vd = q.shape
    nq, kc = blocks * rows, kv.shape[0] * kv.shape[2]
    step = max(1, math.gcd(blocks, 512 // rows))
    qb = step * rows
    kb = math.gcd(kc, 1024)
    wide = lambda r: pl.BlockSpec((r, 2 * qb), lambda i: (0, i))
    whole = lambda a: pl.BlockSpec(a.shape, lambda i: (0, 0))
    kinds = kv.shape[1]
    kind = lambda n: pl.BlockSpec((kv.shape[0], 1, rows, vd), lambda i: (0, n, 0, 0))
    args = [q, kv, kv]
    in_specs = [
        pl.BlockSpec((step, 1, rows, vd), lambda i: (i, 0, 0, 0)),
        kind(kinds - 2),
        kind(kinds - 1),
    ]
    aliases = {}
    if state is not None:
        args += list(state)
        in_specs += [wide(1), wide(1), wide(vd)]
    if final is not None:
        lam, gain = final
        args += [lam, gain]
        in_specs += [pl.BlockSpec(memory_space=pltpu.SMEM), whole(gain)]
        out_shape = jax.ShapeDtypeStruct((nq, vd), jnp.bfloat16)
        out_specs = pl.BlockSpec((qb, vd), lambda i: (i, 0))
    else:
        out_shape = [jax.ShapeDtypeStruct((r, 2 * nq), jnp.float32) for r in (1, 1, vd)]
        out_specs = [wide(1), wide(1), wide(vd)]
        if state is not None:
            aliases = {3: 0, 4: 1, 5: 2}
    scores = 2 * nq * kc
    return pl.pallas_call(
        functools.partial(
            attend_kernel, kb=kb, hd=hd, first=state is None, last=final is not None
        ),
        grid=(nq // qb,),
        in_specs=in_specs,
        out_specs=out_specs,
        out_shape=out_shape,
        input_output_aliases=aliases,
        scratch_shapes=[pltpu.VMEM((vd, kc), jnp.bfloat16)],
        compiler_params=pltpu.CompilerParams(
            dimension_semantics=("arbitrary",), vmem_limit_bytes=VMEM_LIMIT
        ),
        cost_estimate=pl.CostEstimate(
            flops=2 * scores * (hd + vd), transcendentals=scores, bytes_accessed=4 * nq * vd * 4
        ),
    )(*args)


def layer_normed(heads_rows, residual_rows, out_weight, norm_gain):
    branch = jnp.dot(heads_rows, out_weight, preferred_element_type=jnp.float32)
    mixed_in = ALPHA * residual_rows.astype(jnp.float32) + branch
    row_mean = jnp.mean(mixed_in, axis=-1, keepdims=True)
    centered = mixed_in - row_mean
    row_var = jnp.mean(centered * centered, axis=-1, keepdims=True)
    return (centered * lax.rsqrt(row_var + EPSILON) * norm_gain).astype(jnp.bfloat16)


def swap(x, mask):
    group = lax.axis_size("sp")
    return lax.ppermute(x, "sp", [(i, i ^ mask) for i in range(group)])


def subsets(bits):
    return [sum(b for j, b in enumerate(bits) if n >> j & 1) for n in range(1 << len(bits))]


def rank(index, bits):
    return sum((index // b % 2) << j for j, b in enumerate(bits))


def attention(packed, lambdas, head_gain, share_bits, head_bits):
    heads, _, tokens, vd = packed.shape
    peers = [[s + h for h in subsets(head_bits)] for s in subsets(share_bits)]

    def exchange(x):
        return lax.all_to_all(
            x, "sp", split_axis=0, concat_axis=0, axis_index_groups=peers, tiled=True
        )

    mine = exchange(packed)
    chunks = {0: mine[:, 1:]}
    share = 1 << len(share_bits)
    for n in range(1, share):
        low = n & -n
        chunks[n] = swap(chunks[n - low], share_bits[low.bit_length() - 1])
    lam = lax.dynamic_slice_in_dim(lambdas, rank(lax.axis_index("sp"), head_bits), 1)
    final = (lam.reshape(1, 1), head_gain.reshape(vd, 1))
    state = None
    for n in range(share):
        kv = mine if n == 0 else chunks[n]
        state = attend(mine, kv, state, final if n + 1 == share else None, vd // 2)
    back = exchange(state.reshape(heads, tokens, vd))
    return back.transpose(1, 0, 2).reshape(tokens, heads * vd)


def on_device(
    stream,
    query_one,
    key_one,
    query_two,
    key_two,
    values,
    lambdas,
    head_gain,
    out_weight,
    norm_gain,
    gate_weight,
    up_weight,
    down_weight,
):
    heads = lambdas.shape[0]
    group = lax.axis_size("sp")
    device = lax.axis_index("sp")
    far = group // 4
    others = [1 << n for n in range(1, group.bit_length() - 1) if 1 << n != far]
    group_bits = [1, far]
    ordered = group_bits + others
    n_head_bits = heads.bit_length() - 1
    share_bits = ordered[: len(ordered) - n_head_bits]
    head_bits = sorted(ordered[len(ordered) - n_head_bits :])
    place = rank(device, group_bits).reshape(1)
    base = (device - device % 2 - (device // far % 2) * far).reshape(1)

    pieces = pack_weights(place, gate_weight, up_weight, down_weight, 4)
    parts = [pieces[0]]
    for n, mask in ((1, 1), (2, far), (3, far + 1)):
        parts.append(swap(pieces[n], mask))
    block = assemble(place, parts)
    top, lower = others[-1], subsets(others[:-1])[1:]
    weights = {0: block, top: swap(block, top)}
    for mask in lower:
        weights[mask] = swap(block, mask)
    for mask in lower:
        weights[top + mask] = swap(weights[top], mask)

    packed = pack(query_one, query_two, key_one, key_two, values, heads)
    attended = attention(packed, lambdas, head_gain, share_bits, head_bits)
    by_rows = lax.all_to_all(attended, "tp", split_axis=0, concat_axis=1, tiled=True)
    own_normed = layer_normed(by_rows, stream, out_weight, norm_gain)
    own = lax.all_gather(own_normed, "tp", axis=0, tiled=True)

    masks = subsets(others)
    gathered = [weights[mask] for mask in masks]
    near, away = swap(own, 1), swap(own, far)
    near_out, own_out = mixer(base, near, own, gathered, masks, far)
    given = swap(near_out, 1)
    away, own_out = lax.optimization_barrier((away, own_out))
    both = swap(away, 1)
    both_out, away_out = mixer(base, both, away, gathered, masks, far)
    handed = swap(both_out, 1)
    summed = away_out.astype(jnp.float32) + handed.astype(jnp.float32)
    sent = swap(summed.astype(jnp.bfloat16), far)
    partial_terms = (
        own_out.astype(jnp.float32) + given.astype(jnp.float32) + sent.astype(jnp.float32)
    )
    if lax.axis_size("tp") > 1:
        partial_terms = lax.psum_scatter(
            partial_terms.astype(jnp.bfloat16), "tp", scatter_dimension=0, tiled=True
        ).astype(jnp.float32)
    return (ALPHA * own_normed.astype(jnp.float32) + 0.5 * partial_terms).astype(jnp.bfloat16)


def solution(mesh):
    return jax.shard_map(
        on_device,
        mesh=mesh,
        in_specs=(
            P(("sp", "tp"), None),
            P("sp", "tp"),
            P("sp", "tp"),
            P("sp", "tp"),
            P("sp", "tp"),
            P("sp", "tp"),
            P("tp"),
            P(),
            P(),
            P(),
            P("sp", "tp"),
            P("sp", "tp"),
            P("tp", "sp"),
        ),
        out_specs=P(("sp", "tp"), None),
        check_vma=False,
    )
```

```python
import functools
import math

import jax
import jax.numpy as jnp
from jax import lax
from jax.experimental import pallas as pl
from jax.experimental.pallas import tpu as pltpu
from jax.sharding import PartitionSpec as P

ALPHA = 1.4142135623730951
EPSILON = 1e-05
LOG2E = 1.4426950408889634
VMEM_LIMIT = 60 * 1024 * 1024


def pack_kernel(q1, q2, k1, k2, v, out, *, heads, hd, vd):
    for h in range(heads):
        cols = slice(h * hd, (h + 1) * hd)
        out[h, 0] = jnp.concatenate([q1[:, cols], q2[:, cols]], axis=1)
        out[h, 1] = jnp.concatenate([k1[:, cols], k2[:, cols]], axis=1)
        out[h, 2] = v[:, h * vd : (h + 1) * vd]


def pack(q1, q2, k1, k2, v, heads):
    rows = q1.shape[0]
    hd, vd = q1.shape[1] // heads, v.shape[1] // heads
    return pl.pallas_call(
        functools.partial(pack_kernel, heads=heads, hd=hd, vd=vd),
        out_shape=jax.ShapeDtypeStruct((heads, 3, rows, vd), jnp.bfloat16),
        compiler_params=pltpu.CompilerParams(vmem_limit_bytes=VMEM_LIMIT),
    )(q1, q2, k1, k2, v)


def pack_weights_kernel(place, gate, up, down, *outs_and_buf):
    outs, buf = outs_and_buf[:-1], outs_and_buf[-1]
    width = gate.shape[1] // len(outs)
    for p in range(len(outs)):
        cols = slice(p * width, (p + 1) * width)
        slot = jnp.bitwise_xor(place[0], p)
        buf[slot, 0] = gate[:, cols]
        buf[slot, 1] = up[:, cols]
        buf[slot, 2] = down[:, cols]
    for p, out in enumerate(outs):
        out[...] = buf[p]


def pack_weights(place, gate, up, down, parts):
    rows, ff = gate.shape
    piece = (3, rows, ff // parts)
    return pl.pallas_call(
        pack_weights_kernel,
        in_specs=[pl.BlockSpec(memory_space=pltpu.SMEM)] + [pl.BlockSpec()] * 3,
        out_shape=[jax.ShapeDtypeStruct(piece, jnp.bfloat16)] * parts,
        scratch_shapes=[pltpu.VMEM((parts,) + piece, jnp.bfloat16)],
        compiler_params=pltpu.CompilerParams(vmem_limit_bytes=VMEM_LIMIT),
    )(place, gate, up, down)


def assemble_kernel(place, *refs):
    parts, out, buf = refs[:-2], refs[-2], refs[-1]
    rows = parts[0].shape[1]
    for p, part in enumerate(parts):
        at = pl.multiple_of(jnp.bitwise_xor(place[0], p) * rows, rows)
        buf[:, pl.ds(at, rows), :] = part[...]
    for kind in range(out.shape[0]):
        out[kind] = buf[kind].T


def assemble(place, parts):
    kinds, rows, width = parts[0].shape
    block = len(parts) * rows
    return pl.pallas_call(
        assemble_kernel,
        in_specs=[pl.BlockSpec(memory_space=pltpu.SMEM)] + [pl.BlockSpec()] * len(parts),
        out_shape=jax.ShapeDtypeStruct((kinds, width, block), jnp.bfloat16),
        scratch_shapes=[pltpu.VMEM((kinds, block, width), jnp.bfloat16)],
        compiler_params=pltpu.CompilerParams(vmem_limit_bytes=VMEM_LIMIT),
    )(place, *parts)


def mixer_kernel(base, *refs, blocks, strips):
    weights = refs[:blocks]
    xa, xb, out_a, out_b, buf, sems = refs[blocks:]
    block = weights[0].shape[2]

    def copies(part):
        for m in range(blocks):
            at = pl.multiple_of(jnp.bitwise_xor(base[0], m) * block, block)
            yield pltpu.make_async_copy(
                weights[m].at[part],
                buf.at[part, :, pl.ds(at, block)],
                sems.at[part, m],
            )

    for part in range(3):
        for copy in copies(part):
            copy.start()
    rows = [jnp.concatenate([x[:, lo:hi] for lo, hi in strips], axis=1) for x in (xa, xb)]

    def project(x, kind):
        return lax.dot_general(
            x, buf[kind], (((1,), (1,)), ((), ())), preferred_element_type=jnp.float32
        )

    for copy in copies(0):
        copy.wait()
    gates = [project(x, 0) for x in rows]
    for copy in copies(1):
        copy.wait()
    hidden = [
        (gate / (1.0 + jnp.exp(-gate)) * project(x, 1)).astype(jnp.bfloat16)
        for gate, x in zip(gates, rows)
    ]
    for copy in copies(2):
        copy.wait()
    for h, out in zip(hidden, (out_a, out_b)):
        result = jnp.dot(h, buf[2], preferred_element_type=jnp.float32).astype(jnp.bfloat16)
        at = 0
        for lo, hi in strips:
            out[:, lo:hi] = result[:, at : at + hi - lo]
            at += hi - lo


def mixer(base, xa, xb, weights, strips):
    kinds, width, _ = weights[0].shape
    n, d = xa.shape
    return pl.pallas_call(
        functools.partial(mixer_kernel, blocks=len(weights), strips=strips),
        in_specs=[pl.BlockSpec(memory_space=pltpu.SMEM)]
        + [pl.BlockSpec(memory_space=pl.ANY)] * len(weights)
        + [pl.BlockSpec()] * 2,
        out_shape=[jax.ShapeDtypeStruct((n, d), jnp.bfloat16)] * 2,
        scratch_shapes=[
            pltpu.VMEM((kinds, width, d), jnp.bfloat16),
            pltpu.SemaphoreType.DMA((3, len(weights))),
        ],
        compiler_params=pltpu.CompilerParams(vmem_limit_bytes=VMEM_LIMIT),
        cost_estimate=pl.CostEstimate(
            flops=12 * n * d * width,
            transcendentals=2 * n * width,
            bytes_accessed=2 * kinds * d * width,
        ),
    )(base, *weights, xa, xb)


def attend_kernel(*refs, kb, hd, first, last):
    refs = list(refs)
    q_ref, k_ref, v_ref = refs[:3]
    refs = refs[3:]
    if not first:
        m_in, l_in, o_in = refs[:3]
        refs = refs[3:]
    if last:
        lam_ref, gain_ref, out_ref, vt_ref = refs
    else:
        m_out, l_out, o_out, vt_ref = refs
    vd = q_ref.shape[-1]
    qb = q_ref.shape[0] * q_ref.shape[2]
    kc = k_ref.shape[0] * k_ref.shape[2]
    c = LOG2E * hd**-0.5
    keys = k_ref.reshape(kc, vd)

    @pl.when(pl.program_id(0) == 0)
    def _():
        vt_ref[...] = v_ref[...].reshape(kc, vd).T

    qt = q_ref[...].reshape(qb, vd).T
    row = lax.broadcasted_iota(jnp.int32, qt.shape, 0)
    zero = jnp.zeros_like(qt)
    queries = (jnp.where(row < hd, qt, zero), jnp.where(row >= hd, qt, zero))
    state = []
    for a in (0, 1):
        cols = slice(a * qb, (a + 1) * qb)
        if first:
            state.append(
                (
                    jnp.full((1, qb), -1e30, jnp.float32),
                    jnp.zeros((1, qb), jnp.float32),
                    jnp.zeros((vd, qb), jnp.float32),
                )
            )
        else:
            state.append((m_in[:, cols], l_in[:, cols], o_in[:, cols]))

    def scores(step):
        j, a = step
        return jnp.dot(
            keys[j * kb : (j + 1) * kb, :], queries[a], preferred_element_type=jnp.float32
        )

    steps = [(j, a) for j in range(kc // kb) for a in (0, 1)]
    s = scores(steps[0])
    for t, (j, a) in enumerate(steps):
        s_next = scores(steps[t + 1]) if t + 1 < len(steps) else None
        m, l, o = state[a]
        m_new = jnp.maximum(m, jnp.max(s, axis=0, keepdims=True))
        p = jnp.exp2((s - m_new) * c)
        scale = jnp.exp2((m - m_new) * c)
        l = l * scale + jnp.sum(p, axis=0, keepdims=True)
        o = o * scale + jnp.dot(
            vt_ref[:, j * kb : (j + 1) * kb],
            p.astype(jnp.bfloat16),
            preferred_element_type=jnp.float32,
        )
        state[a] = (m_new, l, o)
        s = s_next
    if last:
        first_map = state[0][2] / state[0][1]
        second_map = state[1][2] / state[1][1]
        differ = first_map - lam_ref[0, 0] * second_map
        inverse = lax.rsqrt(jnp.mean(differ * differ, axis=0, keepdims=True) + EPSILON)
        attended = differ * inverse * gain_ref[...] * 0.8
        out_ref[...] = attended.T.astype(jnp.bfloat16)
    else:
        for a in (0, 1):
            cols = slice(a * qb, (a + 1) * qb)
            m_out[:, cols], l_out[:, cols], o_out[:, cols] = state[a]


def attend(q, kv, state, final, hd):
    blocks, _, rows, vd = q.shape
    nq, kc = blocks * rows, kv.shape[0] * kv.shape[2]
    step = max(1, math.gcd(blocks, 512 // rows))
    qb = step * rows
    kb = math.gcd(kc, 1024)
    wide = lambda r: pl.BlockSpec((r, 2 * qb), lambda i: (0, i))
    whole = lambda a: pl.BlockSpec(a.shape, lambda i: (0, 0))
    kinds = kv.shape[1]
    kind = lambda n: pl.BlockSpec((kv.shape[0], 1, rows, vd), lambda i: (0, n, 0, 0))
    args = [q, kv, kv]
    in_specs = [
        pl.BlockSpec((step, 1, rows, vd), lambda i: (i, 0, 0, 0)),
        kind(kinds - 2),
        kind(kinds - 1),
    ]
    aliases = {}
    if state is not None:
        args += list(state)
        in_specs += [wide(1), wide(1), wide(vd)]
    if final is not None:
        lam, gain = final
        args += [lam, gain]
        in_specs += [pl.BlockSpec(memory_space=pltpu.SMEM), whole(gain)]
        out_shape = jax.ShapeDtypeStruct((nq, vd), jnp.bfloat16)
        out_specs = pl.BlockSpec((qb, vd), lambda i: (i, 0))
    else:
        out_shape = [jax.ShapeDtypeStruct((r, 2 * nq), jnp.float32) for r in (1, 1, vd)]
        out_specs = [wide(1), wide(1), wide(vd)]
        if state is not None:
            aliases = {3: 0, 4: 1, 5: 2}
    scores = 2 * nq * kc
    return pl.pallas_call(
        functools.partial(
            attend_kernel, kb=kb, hd=hd, first=state is None, last=final is not None
        ),
        grid=(nq // qb,),
        in_specs=in_specs,
        out_specs=out_specs,
        out_shape=out_shape,
        input_output_aliases=aliases,
        scratch_shapes=[pltpu.VMEM((vd, kc), jnp.bfloat16)],
        compiler_params=pltpu.CompilerParams(
            dimension_semantics=("arbitrary",), vmem_limit_bytes=VMEM_LIMIT
        ),
        cost_estimate=pl.CostEstimate(
            flops=2 * scores * (hd + vd), transcendentals=scores, bytes_accessed=4 * nq * vd * 4
        ),
    )(*args)


def layer_normed(heads_rows, residual_rows, out_weight, norm_gain):
    branch = jnp.dot(heads_rows, out_weight, preferred_element_type=jnp.float32)
    mixed_in = ALPHA * residual_rows.astype(jnp.float32) + branch
    row_mean = jnp.mean(mixed_in, axis=-1, keepdims=True)
    centered = mixed_in - row_mean
    row_var = jnp.mean(centered * centered, axis=-1, keepdims=True)
    return (centered * lax.rsqrt(row_var + EPSILON) * norm_gain).astype(jnp.bfloat16)


def swap(x, mask):
    group = lax.axis_size("sp")
    return lax.ppermute(x, "sp", [(i, i ^ mask) for i in range(group)])


def subsets(bits):
    return [sum(b for j, b in enumerate(bits) if n >> j & 1) for n in range(1 << len(bits))]


def rank(index, bits):
    return sum((index // b % 2) << j for j, b in enumerate(bits))


def attention(packed, lambdas, head_gain, share_bits, head_bits):
    heads, _, tokens, vd = packed.shape
    peers = [[s + h for h in subsets(head_bits)] for s in subsets(share_bits)]

    def exchange(x):
        return lax.all_to_all(
            x, "sp", split_axis=0, concat_axis=0, axis_index_groups=peers, tiled=True
        )

    mine = exchange(packed)
    chunks = {0: mine[:, 1:]}
    share = 1 << len(share_bits)
    for n in range(1, share):
        low = n & -n
        chunks[n] = swap(chunks[n - low], share_bits[low.bit_length() - 1])
    lam = lax.dynamic_slice_in_dim(lambdas, rank(lax.axis_index("sp"), head_bits), 1)
    final = (lam.reshape(1, 1), head_gain.reshape(vd, 1))
    state = None
    for n in range(share):
        kv = mine if n == 0 else chunks[n]
        state = attend(mine, kv, state, final if n + 1 == share else None, vd // 2)
    back = exchange(state.reshape(heads, tokens, vd))
    return back.transpose(1, 0, 2).reshape(tokens, heads * vd)


def on_device(
    stream,
    query_one,
    key_one,
    query_two,
    key_two,
    values,
    lambdas,
    head_gain,
    out_weight,
    norm_gain,
    gate_weight,
    up_weight,
    down_weight,
):
    heads = lambdas.shape[0]
    group = lax.axis_size("sp")
    device = lax.axis_index("sp")
    far = group // 4
    others = [1 << n for n in range(1, group.bit_length() - 1) if 1 << n != far]
    group_bits = [1, far]
    ordered = group_bits + others
    n_head_bits = heads.bit_length() - 1
    share_bits = ordered[: len(ordered) - n_head_bits]
    head_bits = sorted(ordered[len(ordered) - n_head_bits :])
    place = rank(device, group_bits).reshape(1)
    base = rank(device, others).reshape(1)

    pieces = pack_weights(place, gate_weight, up_weight, down_weight.T, 4)
    parts = [pieces[0]]
    for n, mask in ((1, 1), (2, far), (3, far + 1)):
        parts.append(swap(pieces[n], mask))
    block = assemble(place, parts)
    top, lower = others[-1], subsets(others[:-1])[1:]
    weights = {0: block, top: swap(block, top)}
    for mask in lower:
        weights[mask] = swap(block, mask)
    for mask in lower:
        weights[top + mask] = swap(weights[top], mask)

    packed = pack(query_one, query_two, key_one, key_two, values, heads)
    attended = attention(packed, lambdas, head_gain, share_bits, head_bits)
    by_rows = lax.all_to_all(attended, "tp", split_axis=0, concat_axis=1, tiled=True)
    own_normed = layer_normed(by_rows, stream, out_weight, norm_gain)
    own = lax.all_gather(own_normed, "tp", axis=0, tiled=True)

    gathered = [weights[mask] for mask in subsets(others)]
    rows = gate_weight.shape[0]
    strips = [((b + f) * rows, (b + f + 2) * rows) for b in subsets(others) for f in (0, far)]
    near, away = swap(own, 1), swap(own, far)
    both = swap(away, 1)
    both_out, away_out = mixer(base, both, away, gathered, strips)
    handed = swap(both_out, 1)
    summed = away_out.astype(jnp.float32) + handed.astype(jnp.float32)
    sent = swap(summed.astype(jnp.bfloat16), far)
    near_out, own_out = mixer(base, near, own, gathered, strips)
    given = swap(near_out, 1)
    partial_terms = (
        own_out.astype(jnp.float32) + given.astype(jnp.float32) + sent.astype(jnp.float32)
    )
    if lax.axis_size("tp") > 1:
        partial_terms = lax.psum_scatter(
            partial_terms.astype(jnp.bfloat16), "tp", scatter_dimension=0, tiled=True
        ).astype(jnp.float32)
    return (ALPHA * own_normed.astype(jnp.float32) + 0.5 * partial_terms).astype(jnp.bfloat16)


def solution(mesh):
    return jax.shard_map(
        on_device,
        mesh=mesh,
        in_specs=(
            P(("sp", "tp"), None),
            P("sp", "tp"),
            P("sp", "tp"),
            P("sp", "tp"),
            P("sp", "tp"),
            P("sp", "tp"),
            P("tp"),
            P(),
            P(),
            P(),
            P("sp", "tp"),
            P("sp", "tp"),
            P("tp", "sp"),
        ),
        out_specs=P(("sp", "tp"), None),
        check_vma=False,
    )
```

```python
import functools
import math

import jax
import jax.numpy as jnp
from jax import lax
from jax.experimental import pallas as pl
from jax.experimental.pallas import tpu as pltpu
from jax.sharding import PartitionSpec as P

ALPHA = 1.4142135623730951
EPSILON = 1e-05
LOG2E = 1.4426950408889634
VMEM_LIMIT = 60 * 1024 * 1024


def pack_kernel(q1, q2, k1, k2, v, out, *, heads, hd, vd):
    for h in range(heads):
        cols = slice(h * hd, (h + 1) * hd)
        out[h, 0] = jnp.concatenate([q1[:, cols], q2[:, cols]], axis=1)
        out[h, 1] = jnp.concatenate([k1[:, cols], k2[:, cols]], axis=1)
        out[h, 2] = v[:, h * vd : (h + 1) * vd]


def pack(q1, q2, k1, k2, v, heads):
    rows = q1.shape[0]
    hd, vd = q1.shape[1] // heads, v.shape[1] // heads
    return pl.pallas_call(
        functools.partial(pack_kernel, heads=heads, hd=hd, vd=vd),
        out_shape=jax.ShapeDtypeStruct((heads, 3, rows, vd), jnp.bfloat16),
        compiler_params=pltpu.CompilerParams(vmem_limit_bytes=VMEM_LIMIT),
    )(q1, q2, k1, k2, v)


def pack_weights_kernel(place, gate, up, down, *outs_and_buf):
    outs, buf = outs_and_buf[:-1], outs_and_buf[-1]
    width = gate.shape[1] // len(outs)
    for p in range(len(outs)):
        cols = slice(p * width, (p + 1) * width)
        slot = jnp.bitwise_xor(place[0], p)
        buf[slot, 0] = gate[:, cols]
        buf[slot, 1] = up[:, cols]
        buf[slot, 2] = down[:, cols]
    for p, out in enumerate(outs):
        out[...] = buf[p]


def pack_weights(place, gate, up, down, parts):
    rows, ff = gate.shape
    piece = (3, rows, ff // parts)
    return pl.pallas_call(
        pack_weights_kernel,
        in_specs=[pl.BlockSpec(memory_space=pltpu.SMEM)] + [pl.BlockSpec()] * 3,
        out_shape=[jax.ShapeDtypeStruct(piece, jnp.bfloat16)] * parts,
        scratch_shapes=[pltpu.VMEM((parts,) + piece, jnp.bfloat16)],
        compiler_params=pltpu.CompilerParams(vmem_limit_bytes=VMEM_LIMIT),
    )(place, gate, up, down)


def assemble_kernel(place, *refs):
    parts, out, buf = refs[:-2], refs[-2], refs[-1]
    rows = parts[0].shape[1]
    for p, part in enumerate(parts):
        at = pl.multiple_of(jnp.bitwise_xor(place[0], p) * rows, rows)
        buf[:, pl.ds(at, rows), :] = part[...]
    for kind in range(out.shape[0]):
        out[kind] = buf[kind].T


def assemble(place, parts):
    kinds, rows, width = parts[0].shape
    block = len(parts) * rows
    return pl.pallas_call(
        assemble_kernel,
        in_specs=[pl.BlockSpec(memory_space=pltpu.SMEM)] + [pl.BlockSpec()] * len(parts),
        out_shape=jax.ShapeDtypeStruct((kinds, width, block), jnp.bfloat16),
        scratch_shapes=[pltpu.VMEM((kinds, block, width), jnp.bfloat16)],
        compiler_params=pltpu.CompilerParams(vmem_limit_bytes=VMEM_LIMIT),
    )(place, *parts)


def mixer_kernel(base, *refs, blocks, strips):
    weights = refs[:blocks]
    xa, xb, out_a, out_b, buf, sems = refs[blocks:]
    block = weights[0].shape[2]

    def copies(part):
        for m in range(blocks):
            at = pl.multiple_of(jnp.bitwise_xor(base[0], m) * block, block)
            yield pltpu.make_async_copy(
                weights[m].at[part],
                buf.at[part, :, pl.ds(at, block)],
                sems.at[part, m],
            )

    for part in range(3):
        for copy in copies(part):
            copy.start()
    rows = [jnp.concatenate([x[:, lo:hi] for lo, hi in strips], axis=1) for x in (xa, xb)]

    def project(x, kind):
        return lax.dot_general(
            x, buf[kind], (((1,), (1,)), ((), ())), preferred_element_type=jnp.float32
        )

    for copy in copies(0):
        copy.wait()
    gates = [project(x, 0) for x in rows]
    for copy in copies(1):
        copy.wait()
    hidden = [
        (gate / (1.0 + jnp.exp(-gate)) * project(x, 1)).astype(jnp.bfloat16)
        for gate, x in zip(gates, rows)
    ]
    for copy in copies(2):
        copy.wait()
    for h, out in zip(hidden, (out_a, out_b)):
        result = jnp.dot(h, buf[2], preferred_element_type=jnp.float32).astype(jnp.bfloat16)
        at = 0
        for lo, hi in strips:
            out[:, lo:hi] = result[:, at : at + hi - lo]
            at += hi - lo


def mixer(base, xa, xb, weights, strips):
    kinds, width, _ = weights[0].shape
    n, d = xa.shape
    return pl.pallas_call(
        functools.partial(mixer_kernel, blocks=len(weights), strips=strips),
        in_specs=[pl.BlockSpec(memory_space=pltpu.SMEM)]
        + [pl.BlockSpec(memory_space=pl.ANY)] * len(weights)
        + [pl.BlockSpec()] * 2,
        out_shape=[jax.ShapeDtypeStruct((n, d), jnp.bfloat16)] * 2,
        scratch_shapes=[
            pltpu.VMEM((kinds, width, d), jnp.bfloat16),
            pltpu.SemaphoreType.DMA((3, len(weights))),
        ],
        compiler_params=pltpu.CompilerParams(vmem_limit_bytes=VMEM_LIMIT),
        cost_estimate=pl.CostEstimate(
            flops=12 * n * d * width,
            transcendentals=2 * n * width,
            bytes_accessed=2 * kinds * d * width,
        ),
    )(base, *weights, xa, xb)


def attend_kernel(*refs, kb, hd, first, last):
    refs = list(refs)
    q_ref, k_ref, v_ref = refs[:3]
    refs = refs[3:]
    if not first:
        m_in, l_in, o_in = refs[:3]
        refs = refs[3:]
    if last:
        lam_ref, gain_ref, out_ref, vt_ref, keys_one, keys_two = refs
    else:
        m_out, l_out, o_out, vt_ref, keys_one, keys_two = refs
    tripled = (keys_one, keys_two)
    vd = q_ref.shape[-1]
    qb = q_ref.shape[0] * q_ref.shape[2]
    kc = k_ref.shape[0] * k_ref.shape[2]
    c = LOG2E * hd**-0.5

    @pl.when(pl.program_id(0) == 0)
    def _():
        vt_ref[...] = v_ref[...].reshape(kc, vd).T
        keys = k_ref[...].reshape(kc, vd)
        for a, ref in enumerate(tripled):
            own = keys[:, a * hd : (a + 1) * hd]
            ref[...] = jnp.concatenate([own, own, own, jnp.zeros_like(own)], axis=1)

    qt = q_ref[...].reshape(qb, vd).T
    queries = []
    for a in (0, 1):
        exact = qt[a * hd : (a + 1) * hd].astype(jnp.float32) * c
        high = exact.astype(jnp.bfloat16)
        rest = exact - high.astype(jnp.float32)
        middle = rest.astype(jnp.bfloat16)
        low = (rest - middle.astype(jnp.float32)).astype(jnp.bfloat16)
        queries.append(jnp.concatenate([high, middle, low, jnp.zeros_like(high)], axis=0))
    state = []
    for a in (0, 1):
        cols = slice(a * qb, (a + 1) * qb)
        if first:
            state.append(
                (
                    jnp.full((1, qb), -1e30, jnp.float32),
                    jnp.zeros((1, qb), jnp.float32),
                    jnp.zeros((vd, qb), jnp.float32),
                )
            )
        else:
            state.append((m_in[:, cols], l_in[:, cols], o_in[:, cols]))

    def scores(step):
        j, a = step
        return jnp.dot(
            tripled[a][j * kb : (j + 1) * kb, :], queries[a], preferred_element_type=jnp.float32
        )

    steps = [(j, a) for j in range(kc // kb) for a in (0, 1)]
    s = scores(steps[0])
    for t, (j, a) in enumerate(steps):
        s_next = scores(steps[t + 1]) if t + 1 < len(steps) else None
        m, l, o = state[a]
        m_new = jnp.maximum(m, jnp.max(s, axis=0, keepdims=True))
        p = jnp.exp2(s - m_new)
        scale = jnp.exp2(m - m_new)
        l = l * scale + jnp.sum(p, axis=0, keepdims=True)
        o = o * scale + jnp.dot(
            vt_ref[:, j * kb : (j + 1) * kb],
            p.astype(jnp.bfloat16),
            preferred_element_type=jnp.float32,
        )
        state[a] = (m_new, l, o)
        s = s_next
    if last:
        first_map = state[0][2] / state[0][1]
        second_map = state[1][2] / state[1][1]
        differ = first_map - lam_ref[0, 0] * second_map
        inverse = lax.rsqrt(jnp.mean(differ * differ, axis=0, keepdims=True) + EPSILON)
        attended = differ * inverse * gain_ref[...] * 0.8
        out_ref[...] = attended.T.astype(jnp.bfloat16)
    else:
        for a in (0, 1):
            cols = slice(a * qb, (a + 1) * qb)
            m_out[:, cols], l_out[:, cols], o_out[:, cols] = state[a]


def attend(q, kv, state, final, hd):
    blocks, _, rows, vd = q.shape
    nq, kc = blocks * rows, kv.shape[0] * kv.shape[2]
    step = max(1, math.gcd(blocks, 512 // rows))
    qb = step * rows
    kb = math.gcd(kc, 1024)
    wide = lambda r: pl.BlockSpec((r, 2 * qb), lambda i: (0, i))
    whole = lambda a: pl.BlockSpec(a.shape, lambda i: (0, 0))
    kinds = kv.shape[1]
    kind = lambda n: pl.BlockSpec((kv.shape[0], 1, rows, vd), lambda i: (0, n, 0, 0))
    args = [q, kv, kv]
    in_specs = [
        pl.BlockSpec((step, 1, rows, vd), lambda i: (i, 0, 0, 0)),
        kind(kinds - 2),
        kind(kinds - 1),
    ]
    aliases = {}
    if state is not None:
        args += list(state)
        in_specs += [wide(1), wide(1), wide(vd)]
    if final is not None:
        lam, gain = final
        args += [lam, gain]
        in_specs += [pl.BlockSpec(memory_space=pltpu.SMEM), whole(gain)]
        out_shape = jax.ShapeDtypeStruct((nq, vd), jnp.bfloat16)
        out_specs = pl.BlockSpec((qb, vd), lambda i: (i, 0))
    else:
        out_shape = [jax.ShapeDtypeStruct((r, 2 * nq), jnp.float32) for r in (1, 1, vd)]
        out_specs = [wide(1), wide(1), wide(vd)]
        if state is not None:
            aliases = {3: 0, 4: 1, 5: 2}
    scores = 2 * nq * kc
    return pl.pallas_call(
        functools.partial(
            attend_kernel, kb=kb, hd=hd, first=state is None, last=final is not None
        ),
        grid=(nq // qb,),
        in_specs=in_specs,
        out_specs=out_specs,
        out_shape=out_shape,
        input_output_aliases=aliases,
        scratch_shapes=[pltpu.VMEM((vd, kc), jnp.bfloat16)]
        + [pltpu.VMEM((kc, 4 * hd), jnp.bfloat16)] * 2,
        compiler_params=pltpu.CompilerParams(
            dimension_semantics=("arbitrary",), vmem_limit_bytes=VMEM_LIMIT
        ),
        cost_estimate=pl.CostEstimate(
            flops=2 * scores * (hd + vd), transcendentals=scores, bytes_accessed=4 * nq * vd * 4
        ),
    )(*args)


def layer_normed(heads_rows, residual_rows, out_weight, norm_gain):
    branch = jnp.dot(heads_rows, out_weight, preferred_element_type=jnp.float32)
    mixed_in = ALPHA * residual_rows.astype(jnp.float32) + branch
    row_mean = jnp.mean(mixed_in, axis=-1, keepdims=True)
    centered = mixed_in - row_mean
    row_var = jnp.mean(centered * centered, axis=-1, keepdims=True)
    return (centered * lax.rsqrt(row_var + EPSILON) * norm_gain).astype(jnp.bfloat16)


def swap(x, mask):
    group = lax.axis_size("sp")
    return lax.ppermute(x, "sp", [(i, i ^ mask) for i in range(group)])


def subsets(bits):
    return [sum(b for j, b in enumerate(bits) if n >> j & 1) for n in range(1 << len(bits))]


def rank(index, bits):
    return sum((index // b % 2) << j for j, b in enumerate(bits))


def attention(packed, lambdas, head_gain, share_bits, head_bits):
    heads, _, tokens, vd = packed.shape
    peers = [[s + h for h in subsets(head_bits)] for s in subsets(share_bits)]

    def exchange(x):
        return lax.all_to_all(
            x, "sp", split_axis=0, concat_axis=0, axis_index_groups=peers, tiled=True
        )

    mine = exchange(packed)
    chunks = {0: mine[:, 1:]}
    share = 1 << len(share_bits)
    for n in range(1, share):
        low = n & -n
        chunks[n] = swap(chunks[n - low], share_bits[low.bit_length() - 1])
    lam = lax.dynamic_slice_in_dim(lambdas, rank(lax.axis_index("sp"), head_bits), 1)
    final = (lam.reshape(1, 1), head_gain.reshape(vd, 1))
    state = None
    for n in range(share):
        kv = mine if n == 0 else chunks[n]
        state = attend(mine, kv, state, final if n + 1 == share else None, vd // 2)
    back = exchange(state.reshape(heads, tokens, vd))
    return back.transpose(1, 0, 2).reshape(tokens, heads * vd)


def on_device(
    stream,
    query_one,
    key_one,
    query_two,
    key_two,
    values,
    lambdas,
    head_gain,
    out_weight,
    norm_gain,
    gate_weight,
    up_weight,
    down_weight,
):
    heads = lambdas.shape[0]
    group = lax.axis_size("sp")
    device = lax.axis_index("sp")
    far = group // 4
    others = [1 << n for n in range(1, group.bit_length() - 1) if 1 << n != far]
    group_bits = [1, far]
    ordered = group_bits + others
    n_head_bits = heads.bit_length() - 1
    share_bits = ordered[: len(ordered) - n_head_bits]
    head_bits = sorted(ordered[len(ordered) - n_head_bits :])
    place = rank(device, group_bits).reshape(1)
    base = rank(device, others).reshape(1)

    pieces = pack_weights(place, gate_weight, up_weight, down_weight.T, 4)
    parts = [pieces[0]]
    for n, mask in ((1, 1), (2, far), (3, far + 1)):
        parts.append(swap(pieces[n], mask))
    block = assemble(place, parts)
    top, lower = others[-1], subsets(others[:-1])[1:]
    weights = {0: block, top: swap(block, top)}
    for mask in lower:
        weights[mask] = swap(block, mask)
    for mask in lower:
        weights[top + mask] = swap(weights[top], mask)

    packed = pack(query_one, query_two, key_one, key_two, values, heads)
    attended = attention(packed, lambdas, head_gain, share_bits, head_bits)
    by_rows = lax.all_to_all(attended, "tp", split_axis=0, concat_axis=1, tiled=True)
    stream_far = swap(stream, far)
    stream_near = swap(stream, 1)
    stream_both = swap(stream_far, 1)
    rows_far = swap(by_rows, far)
    rows_near = swap(by_rows, 1)
    rows_both = swap(rows_far, 1)

    def normed(heads_rows, residual_rows):
        own = layer_normed(heads_rows, residual_rows, out_weight, norm_gain)
        return own, lax.all_gather(own, "tp", axis=0, tiled=True)

    own_normed, own = normed(by_rows, stream)
    near = normed(rows_near, stream_near)[1]
    away = normed(rows_far, stream_far)[1]
    both = normed(rows_both, stream_both)[1]
    gathered = [weights[mask] for mask in subsets(others)]
    rows = gate_weight.shape[0]
    strips = [((b + f) * rows, (b + f + 2) * rows) for b in subsets(others) for f in (0, far)]
    both_out, away_out = mixer(base, both, away, gathered, strips)
    handed = swap(both_out, 1)
    summed = away_out.astype(jnp.float32) + handed.astype(jnp.float32)
    sent = swap(summed.astype(jnp.bfloat16), far)
    near_out, own_out = mixer(base, near, own, gathered, strips)
    given = swap(near_out, 1)
    partial_terms = (
        own_out.astype(jnp.float32) + given.astype(jnp.float32) + sent.astype(jnp.float32)
    )
    if lax.axis_size("tp") > 1:
        partial_terms = lax.psum_scatter(
            partial_terms.astype(jnp.bfloat16), "tp", scatter_dimension=0, tiled=True
        ).astype(jnp.float32)
    return (ALPHA * own_normed.astype(jnp.float32) + 0.5 * partial_terms).astype(jnp.bfloat16)


def solution(mesh):
    return jax.shard_map(
        on_device,
        mesh=mesh,
        in_specs=(
            P(("sp", "tp"), None),
            P("sp", "tp"),
            P("sp", "tp"),
            P("sp", "tp"),
            P("sp", "tp"),
            P("sp", "tp"),
            P("tp"),
            P(),
            P(),
            P(),
            P("sp", "tp"),
            P("sp", "tp"),
            P("tp", "sp"),
        ),
        out_specs=P(("sp", "tp"), None),
        check_vma=False,
    )
```

```python
import functools
import math

import jax
import jax.numpy as jnp
from jax import lax
from jax.experimental import pallas as pl
from jax.experimental.pallas import tpu as pltpu
from jax.sharding import PartitionSpec as P

ALPHA = 1.4142135623730951
EPSILON = 1e-05
LOG2E = 1.4426950408889634
VMEM_LIMIT = 60 * 1024 * 1024


def pack_kernel(q1, q2, k1, k2, v, out, *, heads, hd, vd):
    for h in range(heads):
        cols = slice(h * hd, (h + 1) * hd)
        out[h, 0] = jnp.concatenate([q1[:, cols], q2[:, cols]], axis=1)
        out[h, 1] = jnp.concatenate([k1[:, cols], k2[:, cols]], axis=1)
        out[h, 2] = v[:, h * vd : (h + 1) * vd]


def pack(q1, q2, k1, k2, v, heads):
    rows = q1.shape[0]
    hd, vd = q1.shape[1] // heads, v.shape[1] // heads
    return pl.pallas_call(
        functools.partial(pack_kernel, heads=heads, hd=hd, vd=vd),
        out_shape=jax.ShapeDtypeStruct((heads, 3, rows, vd), jnp.bfloat16),
        compiler_params=pltpu.CompilerParams(vmem_limit_bytes=VMEM_LIMIT),
    )(q1, q2, k1, k2, v)


def pack_weights_kernel(place, gate, up, down, *outs_and_buf):
    outs, buf = outs_and_buf[:-1], outs_and_buf[-1]
    width = gate.shape[1] // len(outs)
    for p in range(len(outs)):
        cols = slice(p * width, (p + 1) * width)
        slot = jnp.bitwise_xor(place[0], p)
        buf[slot, 0] = gate[:, cols]
        buf[slot, 1] = up[:, cols]
        buf[slot, 2] = down[:, cols]
    for p, out in enumerate(outs):
        out[...] = buf[p]


def pack_weights(place, gate, up, down, parts):
    rows, ff = gate.shape
    piece = (3, rows, ff // parts)
    return pl.pallas_call(
        pack_weights_kernel,
        in_specs=[pl.BlockSpec(memory_space=pltpu.SMEM)] + [pl.BlockSpec()] * 3,
        out_shape=[jax.ShapeDtypeStruct(piece, jnp.bfloat16)] * parts,
        scratch_shapes=[pltpu.VMEM((parts,) + piece, jnp.bfloat16)],
        compiler_params=pltpu.CompilerParams(vmem_limit_bytes=VMEM_LIMIT),
    )(place, gate, up, down)


def assemble_kernel(place, *refs):
    parts, out, buf = refs[:-2], refs[-2], refs[-1]
    rows = parts[0].shape[1]
    for p, part in enumerate(parts):
        at = pl.multiple_of(jnp.bitwise_xor(place[0], p) * rows, rows)
        buf[:, pl.ds(at, rows), :] = part[...]
    for kind in range(out.shape[0]):
        out[kind] = buf[kind].T


def assemble(place, parts):
    kinds, rows, width = parts[0].shape
    block = len(parts) * rows
    return pl.pallas_call(
        assemble_kernel,
        in_specs=[pl.BlockSpec(memory_space=pltpu.SMEM)] + [pl.BlockSpec()] * len(parts),
        out_shape=jax.ShapeDtypeStruct((kinds, width, block), jnp.bfloat16),
        scratch_shapes=[pltpu.VMEM((kinds, block, width), jnp.bfloat16)],
        compiler_params=pltpu.CompilerParams(vmem_limit_bytes=VMEM_LIMIT),
    )(place, *parts)


def mixer_kernel(base, *refs, blocks, strips):
    weights = refs[:blocks]
    xa, xb, out_a, out_b, buf, sems = refs[blocks:]
    block = weights[0].shape[2]

    def copies(part):
        for m in range(blocks):
            at = pl.multiple_of(jnp.bitwise_xor(base[0], m) * block, block)
            yield pltpu.make_async_copy(
                weights[m].at[part],
                buf.at[part, :, pl.ds(at, block)],
                sems.at[part, m],
            )

    for part in range(3):
        for copy in copies(part):
            copy.start()
    rows = [jnp.concatenate([x[:, lo:hi] for lo, hi in strips], axis=1) for x in (xa, xb)]

    def project(x, kind):
        return lax.dot_general(
            x, buf[kind], (((1,), (1,)), ((), ())), preferred_element_type=jnp.float32
        )

    for copy in copies(0):
        copy.wait()
    gates = [project(x, 0) for x in rows]
    for copy in copies(1):
        copy.wait()
    hidden = [
        (gate / (1.0 + jnp.exp(-gate)) * project(x, 1)).astype(jnp.bfloat16)
        for gate, x in zip(gates, rows)
    ]
    for copy in copies(2):
        copy.wait()
    for h, out in zip(hidden, (out_a, out_b)):
        result = jnp.dot(h, buf[2], preferred_element_type=jnp.float32).astype(jnp.bfloat16)
        at = 0
        for lo, hi in strips:
            out[:, lo:hi] = result[:, at : at + hi - lo]
            at += hi - lo


def mixer(base, xa, xb, weights, strips):
    kinds, width, _ = weights[0].shape
    n, d = xa.shape
    return pl.pallas_call(
        functools.partial(mixer_kernel, blocks=len(weights), strips=strips),
        in_specs=[pl.BlockSpec(memory_space=pltpu.SMEM)]
        + [pl.BlockSpec(memory_space=pl.ANY)] * len(weights)
        + [pl.BlockSpec()] * 2,
        out_shape=[jax.ShapeDtypeStruct((n, d), jnp.bfloat16)] * 2,
        scratch_shapes=[
            pltpu.VMEM((kinds, width, d), jnp.bfloat16),
            pltpu.SemaphoreType.DMA((3, len(weights))),
        ],
        compiler_params=pltpu.CompilerParams(vmem_limit_bytes=VMEM_LIMIT),
        cost_estimate=pl.CostEstimate(
            flops=12 * n * d * width,
            transcendentals=2 * n * width,
            bytes_accessed=2 * kinds * d * width,
        ),
    )(base, *weights, xa, xb)


def attend_kernel(*refs, kb, hd, first, last):
    refs = list(refs)
    q_ref, k_ref, v_ref = refs[:3]
    refs = refs[3:]
    if not first:
        m_in, l_in, o_in = refs[:3]
        refs = refs[3:]
    if last:
        lam_ref, gain_ref, out_ref, vt_ref, keys_one, keys_two = refs
    else:
        m_out, l_out, o_out, vt_ref, keys_one, keys_two = refs
    tripled = (keys_one, keys_two)
    vd = q_ref.shape[-1]
    qb = q_ref.shape[0] * q_ref.shape[2]
    kc = k_ref.shape[0] * k_ref.shape[2]
    c = LOG2E * hd**-0.5

    @pl.when(pl.program_id(0) == 0)
    def _():
        vt_ref[...] = v_ref[...].reshape(kc, vd).T
        keys = k_ref[...].reshape(kc, vd)
        for a, ref in enumerate(tripled):
            own = keys[:, a * hd : (a + 1) * hd]
            ref[...] = jnp.concatenate([own, own, own, jnp.zeros_like(own)], axis=1)

    qt = q_ref[...].reshape(qb, vd).T
    queries = []
    for a in (0, 1):
        exact = qt[a * hd : (a + 1) * hd].astype(jnp.float32) * c
        high = exact.astype(jnp.bfloat16)
        rest = exact - high.astype(jnp.float32)
        middle = rest.astype(jnp.bfloat16)
        low = (rest - middle.astype(jnp.float32)).astype(jnp.bfloat16)
        queries.append(jnp.concatenate([high, middle, low, jnp.zeros_like(high)], axis=0))
    state = []
    for a in (0, 1):
        cols = slice(a * qb, (a + 1) * qb)
        if first:
            state.append(
                (
                    jnp.full((1, qb), -1e30, jnp.float32),
                    jnp.zeros((1, qb), jnp.float32),
                    jnp.zeros((vd, qb), jnp.float32),
                )
            )
        else:
            state.append((m_in[:, cols], l_in[:, cols], o_in[:, cols]))

    def scores(step):
        j, a = step
        return jnp.dot(
            tripled[a][j * kb : (j + 1) * kb, :], queries[a], preferred_element_type=jnp.float32
        )

    steps = [(j, a) for j in range(kc // kb) for a in (0, 1)]
    s = scores(steps[0])
    for t, (j, a) in enumerate(steps):
        s_next = scores(steps[t + 1]) if t + 1 < len(steps) else None
        m, l, o = state[a]
        m_new = jnp.maximum(m, jnp.max(s, axis=0, keepdims=True))
        p = jnp.exp2(s - m_new)
        scale = jnp.exp2(m - m_new)
        l = l * scale + jnp.sum(p, axis=0, keepdims=True)
        o = o * scale + jnp.dot(
            vt_ref[:, j * kb : (j + 1) * kb],
            p.astype(jnp.bfloat16),
            preferred_element_type=jnp.float32,
        )
        state[a] = (m_new, l, o)
        s = s_next
    if last:
        first_map = state[0][2] / state[0][1]
        second_map = state[1][2] / state[1][1]
        differ = first_map - lam_ref[0, 0] * second_map
        inverse = lax.rsqrt(jnp.mean(differ * differ, axis=0, keepdims=True) + EPSILON)
        attended = differ * inverse * gain_ref[...] * 0.8
        out_ref[...] = attended.T.astype(jnp.bfloat16)
    else:
        for a in (0, 1):
            cols = slice(a * qb, (a + 1) * qb)
            m_out[:, cols], l_out[:, cols], o_out[:, cols] = state[a]


def attend(q, kv, state, final, hd):
    blocks, _, rows, vd = q.shape
    nq, kc = blocks * rows, kv.shape[0] * kv.shape[2]
    step = max(1, math.gcd(blocks, 512 // rows))
    qb = step * rows
    kb = math.gcd(kc, 1024)
    wide = lambda r: pl.BlockSpec((r, 2 * qb), lambda i: (0, i))
    whole = lambda a: pl.BlockSpec(a.shape, lambda i: (0, 0))
    kinds = kv.shape[1]
    kind = lambda n: pl.BlockSpec((kv.shape[0], 1, rows, vd), lambda i: (0, n, 0, 0))
    args = [q, kv, kv]
    in_specs = [
        pl.BlockSpec((step, 1, rows, vd), lambda i: (i, 0, 0, 0)),
        kind(kinds - 2),
        kind(kinds - 1),
    ]
    aliases = {}
    if state is not None:
        args += list(state)
        in_specs += [wide(1), wide(1), wide(vd)]
    if final is not None:
        lam, gain = final
        args += [lam, gain]
        in_specs += [pl.BlockSpec(memory_space=pltpu.SMEM), whole(gain)]
        out_shape = jax.ShapeDtypeStruct((nq, vd), jnp.bfloat16)
        out_specs = pl.BlockSpec((qb, vd), lambda i: (i, 0))
    else:
        out_shape = [jax.ShapeDtypeStruct((r, 2 * nq), jnp.float32) for r in (1, 1, vd)]
        out_specs = [wide(1), wide(1), wide(vd)]
        if state is not None:
            aliases = {3: 0, 4: 1, 5: 2}
    scores = 2 * nq * kc
    return pl.pallas_call(
        functools.partial(
            attend_kernel, kb=kb, hd=hd, first=state is None, last=final is not None
        ),
        grid=(nq // qb,),
        in_specs=in_specs,
        out_specs=out_specs,
        out_shape=out_shape,
        input_output_aliases=aliases,
        scratch_shapes=[pltpu.VMEM((vd, kc), jnp.bfloat16)]
        + [pltpu.VMEM((kc, 4 * hd), jnp.bfloat16)] * 2,
        compiler_params=pltpu.CompilerParams(
            dimension_semantics=("arbitrary",), vmem_limit_bytes=VMEM_LIMIT
        ),
        cost_estimate=pl.CostEstimate(
            flops=2 * scores * (hd + vd), transcendentals=scores, bytes_accessed=4 * nq * vd * 4
        ),
    )(*args)


def layer_normed(heads_rows, residual_rows, out_weight, norm_gain):
    branch = jnp.dot(heads_rows, out_weight, preferred_element_type=jnp.float32)
    mixed_in = ALPHA * residual_rows.astype(jnp.float32) + branch
    row_mean = jnp.mean(mixed_in, axis=-1, keepdims=True)
    centered = mixed_in - row_mean
    row_var = jnp.mean(centered * centered, axis=-1, keepdims=True)
    return (centered * lax.rsqrt(row_var + EPSILON) * norm_gain).astype(jnp.bfloat16)


def swap(x, mask):
    group = lax.axis_size("sp")
    return lax.ppermute(x, "sp", [(i, i ^ mask) for i in range(group)])


def subsets(bits):
    return [sum(b for j, b in enumerate(bits) if n >> j & 1) for n in range(1 << len(bits))]


def rank(index, bits):
    return sum((index // b % 2) << j for j, b in enumerate(bits))


def attention(packed, lambdas, head_gain, share_bits, head_bits):
    heads, _, tokens, vd = packed.shape
    peers = [[s + h for h in subsets(head_bits)] for s in subsets(share_bits)]

    def exchange(x):
        return lax.all_to_all(
            x, "sp", split_axis=0, concat_axis=0, axis_index_groups=peers, tiled=True
        )

    mine = exchange(packed)
    chunks = {0: mine[:, 1:]}
    share = 1 << len(share_bits)
    for n in range(1, share):
        low = n & -n
        chunks[n] = swap(chunks[n - low], share_bits[low.bit_length() - 1])
    lam = lax.dynamic_slice_in_dim(lambdas, rank(lax.axis_index("sp"), head_bits), 1)
    final = (lam.reshape(1, 1), head_gain.reshape(vd, 1))
    state = None
    for n in range(share):
        kv = mine if n == 0 else chunks[n]
        state = attend(mine, kv, state, final if n + 1 == share else None, vd // 2)
    back = exchange(state.reshape(heads, tokens, vd))
    return back.transpose(1, 0, 2).reshape(tokens, heads * vd)


def on_device(
    stream,
    query_one,
    key_one,
    query_two,
    key_two,
    values,
    lambdas,
    head_gain,
    out_weight,
    norm_gain,
    gate_weight,
    up_weight,
    down_weight,
):
    heads = lambdas.shape[0]
    group = lax.axis_size("sp")
    device = lax.axis_index("sp")
    far = group // 4
    others = [1 << n for n in range(1, group.bit_length() - 1) if 1 << n != far]
    group_bits = [1, far]
    ordered = group_bits + others
    n_head_bits = heads.bit_length() - 1
    share_bits = ordered[: len(ordered) - n_head_bits]
    head_bits = sorted(ordered[len(ordered) - n_head_bits :])
    place = rank(device, group_bits).reshape(1)
    base = rank(device, others).reshape(1)

    pieces = pack_weights(place, gate_weight, up_weight, down_weight.T, 4)
    parts = [pieces[0]]
    for n, mask in ((1, 1), (2, far), (3, far + 1)):
        parts.append(swap(pieces[n], mask))
    block = assemble(place, parts)
    top, lower = others[-1], subsets(others[:-1])[1:]
    weights = {0: block, top: swap(block, top)}
    for mask in lower:
        weights[mask] = swap(block, mask)
    for mask in lower:
        weights[top + mask] = swap(weights[top], mask)

    packed = pack(query_one, query_two, key_one, key_two, values, heads)
    attended = attention(packed, lambdas, head_gain, share_bits, head_bits)
    by_rows = lax.all_to_all(attended, "tp", split_axis=0, concat_axis=1, tiled=True)
    stream_far = swap(stream, far)
    stream_near = swap(stream, 1)
    stream_both = swap(stream_far, 1)
    rows_far = swap(by_rows, far)
    rows_near = swap(by_rows, 1)
    rows_both = swap(rows_far, 1)

    def normed(heads_rows, residual_rows):
        return layer_normed(heads_rows, residual_rows, out_weight, norm_gain)

    def whole(rows):
        return lax.all_gather(rows, "tp", axis=0, tiled=True)

    own_normed = normed(by_rows, stream)
    own, near = whole(own_normed), whole(normed(rows_near, stream_near))
    pair = normed(
        jnp.concatenate([rows_far, rows_both]), jnp.concatenate([stream_far, stream_both])
    )
    away, both = whole(pair[: pair.shape[0] // 2]), whole(pair[pair.shape[0] // 2 :])
    gathered = [weights[mask] for mask in subsets(others)]
    rows = gate_weight.shape[0]
    strips = [((b + f) * rows, (b + f + 2) * rows) for b in subsets(others) for f in (0, far)]
    both_out, away_out = mixer(base, both, away, gathered, strips)
    handed = swap(both_out, 1)
    summed = away_out.astype(jnp.float32) + handed.astype(jnp.float32)
    sent = swap(summed.astype(jnp.bfloat16), far)
    near_out, own_out = mixer(base, near, own, gathered, strips)
    given = swap(near_out, 1)
    partial_terms = (
        own_out.astype(jnp.float32) + given.astype(jnp.float32) + sent.astype(jnp.float32)
    )
    if lax.axis_size("tp") > 1:
        partial_terms = lax.psum_scatter(
            partial_terms.astype(jnp.bfloat16), "tp", scatter_dimension=0, tiled=True
        ).astype(jnp.float32)
    return (ALPHA * own_normed.astype(jnp.float32) + 0.5 * partial_terms).astype(jnp.bfloat16)


def solution(mesh):
    return jax.shard_map(
        on_device,
        mesh=mesh,
        in_specs=(
            P(("sp", "tp"), None),
            P("sp", "tp"),
            P("sp", "tp"),
            P("sp", "tp"),
            P("sp", "tp"),
            P("sp", "tp"),
            P("tp"),
            P(),
            P(),
            P(),
            P("sp", "tp"),
            P("sp", "tp"),
            P("tp", "sp"),
        ),
        out_specs=P(("sp", "tp"), None),
        check_vma=False,
    )
```
